32 devices in a mesh: fs: 8 (over z, x), tp: 4 (over y, core).
Axes of the slice: x: 2, y: 2, z: 4, core: 2. Of those that a mesh axis runs over, the one named last changes fastest.
Arguments:
- saved_input: bfloat16 [49152, 2048], P(('fs', 'tp')), may hold values from -6 to 6
- value_cotangent: bfloat16 [49152, 1024], P(('fs', 'tp')), may hold values from -0.0546875 to 0.0546875
- decay_cotangent: bfloat16 [49152, 16], P(('fs', 'tp')), may hold values from -0.02734375 to 0.02734375
- value_master: float32 [2048, 1024], P('fs', 'tp'), may hold values from -6 to 6
- value_factor: bfloat16 [2048, 256], P('fs'), may hold values from -0.22097087 to 0.22097087
- value_mean: float32 [256, 1024], P('fs', 'tp'), may hold values from -0.625 to 0.625
- value_second: float32 [256, 1024], P('fs', 'tp'), may hold values from 0.0001 to 0.1
- decay_master: float32 [2048, 16], replicated, may hold values from -6 to 6
- decay_mean: float32 [2048, 16], replicated, may hold values from -0.625 to 0.625
- decay_second: float32 [2048, 16], replicated, may hold values from 0.001 to 0.01
Outputs:
- value_step: float32 [2048, 1024], P('fs', 'tp')
- value_new: float32 [2048, 1024], P('fs', 'tp')
- value_copy: bfloat16 [2048, 1024], P(None, 'tp')
- mean_new: float32 [256, 1024], P('fs', 'tp')
- second_new: float32 [256, 1024], P('fs', 'tp')
- decay_step: float32 [2048, 16], replicated
- decay_copy: bfloat16 [2048, 16], replicated
The draws below stay inside these ranges and needn't reach their ends.
All inputs are finite; a program needn't handle non-finite values.
Results may differ from the reference program's by a relative error of at most 0.0004.
Values may be sent and summed in bfloat16 or wider, within the bound.
A program may use at most 64 MiB of HBM per device.

```python
import math
import jax
import jax.numpy as jnp
from jax import lax

D = 2048
HG = 16
GW = 1024
RANK = 256
TOKENS = 49152


def draw_value_factor(key, part):
    base_key, tilt_key = jax.random.split(jax.random.fold_in(key, 17))
    base = jnp.clip(jax.random.normal(base_key, (D, RANK), jnp.float32), -4.0, 4.0)
    place = jnp.arange(D, dtype=jnp.float32)[:, None] / D
    jitter = jax.random.uniform(tilt_key, (D, 1), jnp.float32)
    scale = 10.0 ** (0.5 * place + 0.5 * jitter) * 0.25 * D ** (-0.5)
    return (base * scale).astype(jnp.bfloat16)


def draw_value_second(key, part):
    entry_key, tilt_key = jax.random.split(jax.random.fold_in(key, 29))
    place = jnp.arange(GW, dtype=jnp.float32)[None, :] / GW
    jitter = jax.random.uniform(tilt_key, (1, GW), jnp.float32)
    column = 100.0 ** (0.5 * place + 0.5 * jitter)
    entry = 10.0 ** jax.random.uniform(entry_key, (RANK, GW), jnp.float32)
    return (0.0001 * entry * column).astype(jnp.float32)


def strengthened(result, own_key, source, target, parts, factor):
    owner, partner = [(jnp.arange(result.shape[axis_at]) // (result.shape[axis_at] // parts)).reshape([-1 if axis == axis_at else 1 for axis in range(result.ndim)]) for axis_at in (source, target)]
    chosen = jax.random.permutation(own_key, parts)[partner]
    strong = (owner == chosen) | (owner == (partner + parts // 2) % parts)
    return jnp.where(strong, factor * result, result)


def shard_levels(stream_key, extent, cuts, smallest, largest):
    def one(position, blocks):
        steps = jax.random.uniform(jax.random.fold_in(jax.random.fold_in(stream_key, 6), position), (blocks,), jnp.float32, smallest / len(cuts), largest / len(cuts))
        return jnp.repeat(jnp.exp(steps), extent[position] // blocks).reshape((-1,) + (1,) * (len(extent) - position - 1))

    level = one(*cuts[0])
    for cut in cuts[1:]:
        level = level * one(*cut)
    return level


def centred(stream_key, dims, spread, reach, pieces=(), kind=jnp.bfloat16):
    drawn = spread * jax.random.normal(stream_key, dims, jnp.float32)
    if pieces:
        drawn = drawn * shard_levels(stream_key, dims, pieces, -0.22, 0.18)
    return jnp.clip(drawn, -reach, reach).astype(kind)


def bell_draw_with(own_key, extent, deviation, bound, shards, heavy, kind=jnp.bfloat16):
    drawn = deviation * jax.random.normal(own_key, extent, jnp.float32)
    if shards:
        drawn = drawn * shard_levels(own_key, extent, shards, -0.22, 0.18)
    return jnp.clip(strengthened(drawn, jax.random.fold_in(own_key, 3), *heavy), -bound, bound).astype(kind)


def setup_inputs(seed: int = 0) -> dict:
    key_list = jax.random.split(jax.random.key(seed), 11)
    return {
        "saved_input": centred(key_list[0], (TOKENS, D), 1.0, 6.0, ((0, 32),)),
        "value_cotangent": bell_draw_with(key_list[1], (TOKENS, GW), (TOKENS ** -0.5), 0.0546875, ((0, 32),), (0, 1, 32, 2.75)),
        "decay_cotangent": centred(key_list[2], (TOKENS, HG), (TOKENS ** -0.5), 0.02734375, ((0, 32),)),
        "value_master": centred(key_list[3], (D, GW), 1.0, 6.0, ((0, 8), (1, 4)), jnp.float32),
        "value_factor": draw_value_factor(jax.random.fold_in(key_list[10], 71), 0),
        "value_mean": centred(key_list[5], (RANK, GW), 0.1, 0.625, ((0, 8), (1, 4)), jnp.float32),
        "value_second": draw_value_second(jax.random.fold_in(key_list[10], 71), 0),
        "decay_master": centred(key_list[7], (D, HG), 1.0, 6.0, (), jnp.float32),
        "decay_mean": centred(key_list[8], (D, HG), 0.1, 0.625, (), jnp.float32),
        "decay_second": jnp.clip(jnp.exp(jax.random.uniform(key_list[9], (D, HG), jnp.float32, math.log(0.001), math.log(0.01))), 0.001, 0.01),
    }


BETA_ONE = 0.9
BETA_TWO = 0.99
ADAM_EPS = 1e-08
RMS_EPS = 1e-06
LEARN_RATE = 0.05
TOKEN_DIMS = (((0,), (0,)), ((), ()))

def adam_direction(moment_one, moment_two, gradient):
    mean_new = BETA_ONE * moment_one + (1.0 - BETA_ONE) * gradient
    second_new = BETA_TWO * moment_two + (1.0 - BETA_TWO) * gradient * gradient
    return (mean_new, second_new, mean_new / (jnp.sqrt(second_new) + ADAM_EPS))

def reference(saved_input, value_cotangent, decay_cotangent, value_master, value_factor, value_mean, value_second, decay_master, decay_mean, decay_second):
    value_grad = lax.dot_general(saved_input, value_cotangent, TOKEN_DIMS, preferred_element_type=jnp.float32)
    factor_wide = value_factor.astype(jnp.float32)
    projected = lax.dot_general(factor_wide, value_grad, TOKEN_DIMS, precision=lax.Precision.HIGHEST, preferred_element_type=jnp.float32)
    mean_new, second_new, direction = adam_direction(value_mean, value_second, projected)
    raw_update = jnp.dot(factor_wide, direction, precision=lax.Precision.HIGHEST, preferred_element_type=jnp.float32)
    value_step = raw_update * lax.rsqrt(jnp.mean(raw_update * raw_update) + RMS_EPS)
    value_new = value_master - LEARN_RATE * value_step
    value_copy = value_new.astype(jnp.bfloat16)
    decay_grad = lax.dot_general(saved_input, decay_cotangent, TOKEN_DIMS, preferred_element_type=jnp.float32)
    unused_mean, unused_second, decay_step = adam_direction(decay_mean, decay_second, decay_grad)
    decay_copy = (decay_master - LEARN_RATE * decay_step).astype(jnp.bfloat16)
    return (value_step, value_new, value_copy, mean_new, second_new, decay_step, decay_copy)
```

```python
import functools

import jax
import jax.numpy as jnp
from jax import lax
from jax.experimental import pallas as pl
from jax.experimental.pallas import tpu as pltpu
from jax.sharding import PartitionSpec as P

BETA_ONE = 0.9
BETA_TWO = 0.99
ADAM_EPS = 1e-08
RMS_EPS = 1e-06
LEARN_RATE = 0.05
LANES = 128
BF16 = jnp.bfloat16
F32 = jnp.float32


def flip(index, bits):
    result = index
    place = 1
    while place <= bits:
        if bits & place:
            result = result + place - 2 * place * ((index // place) % 2)
        place *= 2
    return result


def adam(moment_one, moment_two, gradient):
    mean_new = BETA_ONE * moment_one + (1.0 - BETA_ONE) * gradient
    second_new = BETA_TWO * moment_two + (1.0 - BETA_TWO) * gradient * gradient
    return mean_new, second_new, mean_new / (jnp.sqrt(second_new) + ADAM_EPS)


def dot(left, right):
    return jnp.dot(left, right, preferred_element_type=F32)


def kernel(
    fs_n, tp_n,
    x_hbm, c_hbm, dc_hbm, master_hbm, factor_hbm, mean_hbm, second_hbm,
    dmaster_hbm, dmean_hbm, dsecond_hbm,
    step_v, new_v, copy_v, mean_v, second_v, dstep_v, dcopy_v,
    x, c_in, dc, master, factor, mean, second, dmaster, dmean, dsecond,
    mapped, high, low, pa, pb, ra1, rb1, ra2, rb2, ra3, rb3, zed, rz,
    direction, squares, sq_tp,
    dpart, dr_tp, dmid, dr_fs, dgrad,
    in_sem,
    fz_s, fz_r, fx_s, fx_r, fc_s, fc_r,
    p1_s, p1_r, a2_s, a2_r, b2_s, b2_r, a3_s, a3_r, b3_s, b3_r, z_s, z_r,
    dz_s, dz_r, dx_s, dx_r, q1_s, q1_r, vz_s, vz_r, vx_s, vx_r,
    e1_s, e1_r, e2_s, e2_r, e3_s, e3_r, e4_s, e4_r,
):
    fs = lax.axis_index("fs")
    tp = lax.axis_index("tp")
    core = tp % 2
    other = 1 - core
    high_tp = tp // 2
    lo = fs % 2
    hi = fs // 2
    y_n = tp_n // 2
    h_n = fs_n // 2
    half_n = h_n // 2
    rows = factor.shape[0] // fs_n
    part = rows // 2
    rank_rows, width = mean.shape
    tokens, depth = x.shape
    sends = []

    def send(src, dst, ssem, rsem, device):
        copy = pltpu.make_async_remote_copy(
            src_ref=src, dst_ref=dst, send_sem=ssem, recv_sem=rsem,
            device_id=device, device_id_type=pl.DeviceIdType.MESH)
        copy.start()
        sends.append(copy)

    def arrive(dst, ssem, rsem, device):
        pltpu.make_async_remote_copy(
            src_ref=dst, dst_ref=dst, send_sem=ssem, recv_sem=rsem,
            device_id=device, device_id_type=pl.DeviceIdType.MESH).wait_recv()

    x_peer = (flip(fs, 1), tp)
    core_peer = (fs, flip(tp, 1))

    def z_peer(d):
        return (flip(hi, d) * 2 + lo, tp)

    def y_peer(d):
        return (fs, flip(high_tp, d) * 2 + core)

    def tp_peer(d):
        return (fs, flip(tp, d))

    def fs_peer(d):
        return (flip(fs, d), tp)

    def block(ref, index, size):
        return ref.at[pl.ds(pl.multiple_of(index * size, size), size)]

    def piece(index, which):
        return factor.at[pl.ds(pl.multiple_of(index * rows + which * part, part), part)]

    ins = [
        (factor_hbm, block(factor, fs, rows)), (dc_hbm, dc), (x_hbm, x), (c_hbm, c_in),
        (mean_hbm, mean), (second_hbm, second), (master_hbm, master),
        (dmean_hbm, dmean), (dsecond_hbm, dsecond), (dmaster_hbm, dmaster),
    ]
    loads = [pltpu.make_async_copy(s, d, in_sem.at[i]) for i, (s, d) in enumerate(ins)]
    for load in loads:
        load.start()

    barrier = pltpu.get_barrier_semaphore()
    for d in range(1, tp_n):
        pl.semaphore_signal(barrier, inc=1, device_id=tp_peer(d), device_id_type=pl.DeviceIdType.MESH)
    for d in range(1, fs_n):
        pl.semaphore_signal(barrier, inc=1, device_id=fs_peer(d), device_id_type=pl.DeviceIdType.MESH)
    pl.semaphore_wait(barrier, tp_n + fs_n - 2)

    loads[0].wait()
    mine = piece(fs, core)
    send(mine, mine, fx_s.at[0], fx_r.at[0], x_peer)
    for d in range(1, h_n):
        send(mine, mine, fz_s.at[d], fz_r.at[d], z_peer(d))

    def forward_z(d):
        ref = piece(flip(hi, d) * 2 + lo, core)
        arrive(ref, fz_s.at[d], fz_r.at[d], z_peer(d))
        send(ref, ref, fx_s.at[d], fx_r.at[d], x_peer)
        send(ref, ref, fc_s.at[0, d], fc_r.at[0, d], core_peer)

    def forward_x(d):
        ref = piece(flip(hi, d) * 2 + 1 - lo, core)
        arrive(ref, fx_s.at[d], fx_r.at[d], x_peer)
        send(ref, ref, fc_s.at[1, d], fc_r.at[1, d], core_peer)

    def arrive_core(d):
        for side in range(2):
            if side == 0 and d == 0:
                continue
            ref = piece(flip(hi, d) * 2 + (lo if side == 0 else 1 - lo), other)
            arrive(ref, fc_s.at[side, d], fc_r.at[side, d], core_peer)

    loads[1].wait()
    turned = dc[...]
    heads = turned.shape[0]
    unit = dpart.shape[2]
    loads[2].wait()
    for d in range(1, half_n):
        forward_z(d)
    forward_x(0)

    lane_tile = 2 * LANES
    for tile in range(depth // lane_tile):
        value = dot(turned, x[:, tile * lane_tile:(tile + 1) * lane_tile])
        for k in range(lane_tile // LANES):
            for h in range(0, heads, unit):
                b = ((tile * (lane_tile // LANES) + k) * heads + h) // unit
                dpart[b // fs_n, b % fs_n] = value[h:h + unit, k * LANES:(k + 1) * LANES]
    for d in range(1, tp_n):
        send(dpart.at[flip(tp, d)], dr_tp.at[d], e1_s.at[d], e1_r.at[d], tp_peer(d))

    for d in range(half_n, h_n):
        forward_z(d)
    for d in range(1, half_n):
        forward_x(d)
    for d in range(half_n):
        arrive_core(d)

    span = depth // 2
    near = hi // half_n
    tall = tokens // 6 if tokens % 6 == 0 else tokens

    def columns(which):
        return pl.ds(pl.multiple_of(which * span, span), span)

    near_cols, far_cols = columns(near), columns(1 - near)

    @pl.loop(0, tokens // tall)
    def _(i):
        r = pl.ds(pl.multiple_of(i * tall, tall), tall)
        mapped[r, :] = dot(x[r, near_cols], factor[near_cols, :])

    for d in range(half_n, h_n):
        forward_x(d)
    for d in range(half_n, h_n):
        arrive_core(d)

    @pl.loop(0, tokens // tall)
    def _(i):
        r = pl.ds(pl.multiple_of(i * tall, tall), tall)
        full = mapped[r, :] + dot(x[r, far_cols], factor[far_cols, :])
        full = jnp.transpose(full)
        top = full.astype(BF16)
        high[:, r] = top
        low[:, r] = (full - top.astype(F32)).astype(BF16)

    loads[3].wait()

    def chunk(c, y):
        cols = pl.ds(pl.multiple_of((y * 2 + c) * width, width), width)
        value = dot(high[...], c_in[:, cols]) + dot(low[...], c_in[:, cols])
        for f in range(fs_n):
            block_value = value[f * rank_rows:(f + 1) * rank_rows]
            h, xx = f // 2, f % 2
            if h < half_n:
                pa[c, y, xx, h] = block_value
            else:
                pb[c, xx, y, h - half_n] = block_value

    for y in range(y_n):
        chunk(other, y)
        send(pa.at[other, y], ra1.at[y], p1_s.at[0, y], p1_r.at[0, y], core_peer)
        send(pb.at[other, :, y], rb1.at[:, y], p1_s.at[1, y], p1_r.at[1, y], core_peer)

    for d in range(1, tp_n):
        arrive(dr_tp.at[d], e1_s.at[d], e1_r.at[d], tp_peer(d))
    total = dpart[tp]
    for d in range(1, tp_n):
        total = total + dr_tp[d]
    dmid[...] = total
    for d in range(1, fs_n):
        send(dmid.at[flip(fs, d)], dr_fs.at[d], e2_s.at[d], e2_r.at[d], fs_peer(d))

    for y in range(y_n):
        chunk(core, y)
    for y in range(y_n):
        arrive(ra1.at[y], p1_s.at[0, y], p1_r.at[0, y], core_peer)
        arrive(rb1.at[:, y], p1_s.at[1, y], p1_r.at[1, y], core_peer)
    pb[core] = pb[core] + rb1[...]
    send(pb.at[core, 1 - lo], rb2, b2_s, b2_r, x_peer)
    pa[core] = pa[core] + ra1[...]
    for d in range(1, y_n):
        send(pa.at[core, flip(high_tp, d)], ra2.at[d], a2_s.at[d], a2_r.at[d], y_peer(d))

    for d in range(1, fs_n):
        arrive(dr_fs.at[d], e2_s.at[d], e2_r.at[d], fs_peer(d))
    tile_sum = dmid[fs]
    for d in range(1, fs_n):
        tile_sum = tile_sum + dr_fs[d]
    dgrad[tp, fs] = tile_sum
    own_tile = dgrad.at[tp, fs]
    for d in range(1, fs_n):
        send(own_tile, own_tile, e3_s.at[d], e3_r.at[d], fs_peer(d))

    for d in range(1, y_n):
        arrive(ra2.at[d], a2_s.at[d], a2_r.at[d], y_peer(d))
    value = pa[core, high_tp]
    for d in range(1, y_n):
        value = value + ra2[d]
    pa[core, high_tp] = value
    send(pa.at[core, high_tp, 1 - lo], ra3, a3_s, a3_r, x_peer)
    arrive(rb2, b2_s, b2_r, x_peer)
    pb[core, lo] = pb[core, lo] + rb2[...]
    for d in range(1, y_n):
        send(pb.at[core, lo, flip(high_tp, d)], rb3.at[d], b3_s.at[d], b3_r.at[d], y_peer(d))

    arrive(ra3, a3_s, a3_r, x_peer)
    zed[0:half_n] = pa[core, high_tp, lo] + ra3[...]
    for d in range(1, y_n):
        arrive(rb3.at[d], b3_s.at[d], b3_r.at[d], y_peer(d))
    value = pb[core, lo, high_tp]
    for d in range(1, y_n):
        value = value + rb3[d]
    zed[half_n:h_n] = value
    for d in reversed(range(1, h_n)):
        send(zed.at[flip(hi, d)], rz.at[d], z_s.at[d], z_r.at[d], z_peer(d))

    for d in range(1, fs_n):
        ref = dgrad.at[tp, flip(fs, d)]
        arrive(ref, e3_s.at[d], e3_r.at[d], fs_peer(d))
    own_row = dgrad.at[tp]
    for d in range(1, tp_n):
        send(own_row, own_row, e4_s.at[d], e4_r.at[d], tp_peer(d))

    loads[4].wait()
    loads[5].wait()
    loads[6].wait()
    for d in range(1, h_n):
        arrive(rz.at[d], z_s.at[d], z_r.at[d], z_peer(d))
    projected = zed[hi]
    for d in range(1, h_n):
        projected = projected + rz[d]

    mean_new, second_new, own_direction = adam(mean[...], second[...], projected)
    own_dir = block(direction, fs, rank_rows)
    direction[pl.ds(pl.multiple_of(fs * rank_rows, rank_rows), rank_rows), :] = own_direction
    for d in reversed(range(1, h_n)):
        send(own_dir, own_dir, dz_s.at[d], dz_r.at[d], z_peer(d))
    send(own_dir, own_dir, dx_s.at[0], dx_r.at[0], x_peer)
    mean_v[...] = mean_new
    second_v[...] = second_new
    for d in range(1, h_n):
        ref = block(direction, flip(hi, d) * 2 + lo, rank_rows)
        arrive(ref, dz_s.at[d], dz_r.at[d], z_peer(d))
        send(ref, ref, dx_s.at[d], dx_r.at[d], x_peer)
    for d in range(h_n):
        ref = block(direction, flip(hi, d) * 2 + 1 - lo, rank_rows)
        arrive(ref, dx_s.at[d], dx_r.at[d], x_peer)

    whole = direction[...]
    whole_top = whole.astype(BF16)
    whole_low = (whole - whole_top.astype(F32)).astype(BF16)
    own_rows = pl.ds(pl.multiple_of(fs * rows, rows), rows)

    def update(r):
        return dot(factor[r, :], whole_top) + dot(factor[r, :], whole_low)

    squares[...] = jnp.zeros_like(squares)

    @pl.loop(0, fs_n)
    def _(i):
        raw = update(pl.ds(pl.multiple_of(i * rows, rows), rows))
        squares[...] += jnp.sum((raw * raw).reshape(rows // 8, 8, width), axis=0)

    for d in range(1, tp_n):
        send(squares, sq_tp.at[d], q1_s.at[d], q1_r.at[d], tp_peer(d))
    step_v[...] = update(own_rows)
    total = squares[...]
    for d in range(1, tp_n):
        arrive(sq_tp.at[d], q1_s.at[d], q1_r.at[d], tp_peer(d))
        total = total + sq_tp[d]
    total = jnp.sum(jnp.sum(total, axis=0, keepdims=True), axis=1, keepdims=True)
    scale = lax.rsqrt(total / (depth * width * tp_n) + RMS_EPS)
    value_step = step_v[...] * scale
    value_new = master[...] - LEARN_RATE * value_step
    copy_v[own_rows, :] = value_new.astype(BF16)
    own_copy = block(copy_v, fs, rows)
    send(own_copy, own_copy, vx_s.at[0], vx_r.at[0], x_peer)
    for d in range(1, h_n):
        send(own_copy, own_copy, vz_s.at[d], vz_r.at[d], z_peer(d))
    step_v[...] = value_step
    new_v[...] = value_new

    def forward_copy(d):
        index = flip(hi, d) * 2 + lo
        ref = block(copy_v, index, rows)
        arrive(ref, vz_s.at[d], vz_r.at[d], z_peer(d))
        send(ref, ref, vx_s.at[d], vx_r.at[d], x_peer)

    for d in range(1, tp_n):
        ref = dgrad.at[flip(tp, d)]
        arrive(ref, e4_s.at[d], e4_r.at[d], tp_peer(d))
    for load in loads[7:]:
        load.wait()
    per_lane = heads // unit
    forward_at = {}
    blocks = depth // LANES
    for d in range(1, h_n):
        forward_at.setdefault(min(blocks - 1, d * blocks // h_n), []).append(d)
    for lane in range(blocks):
        tiles = []
        for k in range(per_lane):
            b = lane * per_lane + k
            tiles.append(dgrad[b // fs_n, b % fs_n])
        grad = jnp.concatenate(tiles, axis=0)
        r = slice(lane * LANES, (lane + 1) * LANES)
        unused_mean, unused_second, dstep = adam(dmean[:, r], dsecond[:, r], grad)
        dstep_v[:, r] = dstep
        dcopy_v[:, r] = (dmaster[:, r] - LEARN_RATE * dstep).astype(BF16)
        for d in forward_at.get(lane, ()):
            forward_copy(d)
    for d in range(h_n):
        ref = block(copy_v, flip(hi, d) * 2 + 1 - lo, rows)
        arrive(ref, vx_s.at[d], vx_r.at[d], x_peer)
    for copy in sends:
        copy.wait_send()


def write_out(*refs):
    held, outs, sem = refs[:7], refs[7:14], refs[14]
    copies = [pltpu.make_async_copy(h, o, sem.at[i]) for i, (h, o) in enumerate(zip(held, outs))]
    for copy in copies:
        copy.start()
    for copy in copies:
        copy.wait()


def local(fs_n, tp_n, *args):
    x, c_in, dc, master, factor, mean, second, dmaster, dmean, dsecond = args
    rows, rank = factor.shape
    rank_rows, width = mean.shape
    tokens, depth = x.shape
    dc, dmaster, dmean, dsecond = dc.T, dmaster.T, dmean.T, dsecond.T
    args = (x, c_in, dc, master, factor, mean, second, dmaster, dmean, dsecond)
    heads = dc.shape[0]
    h_n, y_n = fs_n // 2, tp_n // 2
    half_n = h_n // 2
    unit = heads * (depth // LANES) // (fs_n * tp_n)
    v = pltpu.VMEM
    shape = jax.ShapeDtypeStruct
    dma = lambda *n: pltpu.SemaphoreType.DMA(n)
    pair = lambda *n: [dma(*n), dma(*n)]
    single = [pltpu.SemaphoreType.DMA, pltpu.SemaphoreType.DMA]
    scratch = [
        v(x.shape, BF16), v(c_in.shape, BF16), v(dc.shape, BF16), v(master.shape, F32),
        v((depth, rank), BF16), v(mean.shape, F32), v(second.shape, F32),
        v(dmaster.shape, F32), v(dmean.shape, F32), v(dsecond.shape, F32),
        v((tokens, rank), F32), v((rank, tokens), BF16), v((rank, tokens), BF16),
        v((2, y_n, 2, half_n, rank_rows, width), F32),
        v((2, 2, y_n, half_n, rank_rows, width), F32),
        v((y_n, 2, half_n, rank_rows, width), F32),
        v((2, y_n, half_n, rank_rows, width), F32),
        v((y_n, 2, half_n, rank_rows, width), F32),
        v((y_n, half_n, rank_rows, width), F32),
        v((half_n, rank_rows, width), F32),
        v((y_n, half_n, rank_rows, width), F32),
        v((h_n, rank_rows, width), F32), v((h_n, rank_rows, width), F32),
        v((rank, width), F32), v((8, width), F32), v((tp_n, 8, width), F32),
        v((tp_n, fs_n, unit, LANES), F32), v((tp_n, fs_n, unit, LANES), F32),
        v((fs_n, unit, LANES), F32), v((fs_n, unit, LANES), F32),
        v((tp_n, fs_n, unit, LANES), F32),
        dma(10),
        *pair(h_n), *pair(h_n), *pair(2, h_n),
        *pair(2, y_n), *pair(y_n), *single, *single, *pair(y_n), *pair(h_n),
        *pair(h_n), *pair(h_n), *pair(tp_n), *pair(h_n), *pair(h_n),
        *pair(tp_n), *pair(fs_n), *pair(fs_n), *pair(tp_n),
    ]
    results = (
        (master.shape, F32), (master.shape, F32), ((depth, width), BF16),
        (mean.shape, F32), (mean.shape, F32), (dmean.shape, F32), (dmean.shape, BF16),
    )
    held = pl.pallas_call(
        functools.partial(kernel, fs_n, tp_n),
        out_shape=tuple(v(*r) for r in results),
        in_specs=[pl.BlockSpec(memory_space=pl.ANY)] * 10,
        out_specs=[pl.BlockSpec(memory_space=v)] * 7,
        scratch_shapes=scratch,
        compiler_params=pltpu.CompilerParams(
            collective_id=0, has_side_effects=True, vmem_limit_bytes=48 * 1024 * 1024),
    )(*[pltpu.with_memory_space_constraint(a, pltpu.HBM) for a in args])
    held = [pltpu.with_memory_space_constraint(h, v) for h in held]
    outs = pl.pallas_call(
        write_out,
        out_shape=tuple(shape(*r) for r in results),
        in_specs=[pl.BlockSpec(memory_space=v)] * 7,
        out_specs=[pl.BlockSpec(memory_space=pl.ANY)] * 7,
        scratch_shapes=[dma(7)],
        compiler_params=pltpu.CompilerParams(vmem_limit_bytes=1024 * 1024),
    )(*held)
    return (*outs[:5], outs[5].T, outs[6].T)


def solution(mesh):
    split = P(("fs", "tp"), None)
    in_specs = (split, split, split, P("fs", "tp"), P("fs", None), P("fs", "tp"), P("fs", "tp"), P(), P(), P())
    out_specs = (P("fs", "tp"), P("fs", "tp"), P(None, "tp"), P("fs", "tp"), P("fs", "tp"), P(), P())
    body = functools.partial(local, mesh.shape["fs"], mesh.shape["tp"])
    return jax.shard_map(body, mesh=mesh, in_specs=in_specs, out_specs=out_specs, check_vma=False)
```
